512 devices in a mesh: sp: 64 (over z, y), tp: 8 (over x, core).
Axes of the slice: x: 4, y: 4, z: 16, core: 2. Of those that a mesh axis runs over, the one named last changes fastest.
Arguments:
- tokens: bfloat16 [8192, 4096], P('sp'), may hold values from -6 to 6
- norm_gain: bfloat16 [4096], replicated, may hold values from 0.099609375 to 1.8984375
- w_pool_in: bfloat16 [4096, 1024], P('sp', 'tp'), may hold values from -0.09375 to 0.09375
- w_x: bfloat16 [4096, 2048], P('sp', 'tp'), may hold values from -0.09375 to 0.09375
- w_z: bfloat16 [4096, 2048], P('sp', 'tp'), may hold values from -0.09375 to 0.09375
- w_b: bfloat16 [4096, 1024], P('sp', 'tp'), may hold values from -0.09375 to 0.09375
- w_c: bfloat16 [4096, 1024], P('sp', 'tp'), may hold values from -0.09375 to 0.09375
- w_dt: bfloat16 [4096, 2, 32], P(None, None, 'tp'), may hold values from -0.09375 to 0.09375
- conv_x: bfloat16 [3, 2048], P(None, 'tp'), may hold values from -3.5 to 3.5
- conv_b: bfloat16 [3, 1024], P(None, 'tp'), may hold values from -3.5 to 3.5
- output_map_taps: bfloat16 [3, 1024], P(None, 'tp'), may hold values from -3.5 to 3.5
- decay_log: float32 [2, 32], P(None, 'tp'), may hold values from -16 to 0
- leak: float32 [8192, 2, 32], P('sp', None, 'tp'), may hold values from 0 to 2
- init_state: float32 [2, 32, 64, 128], P(None, 'tp'), may hold values from -162.9174 to 162.9174
- head_gain: bfloat16 [2048], P('tp'), may hold values from 0.099609375 to 1.8984375
- w_out: bfloat16 [3072, 4096], P('sp', 'tp'), may hold values from -0.109375 to 0.109375
Outputs:
- mixed: bfloat16 [8192, 4096], P('sp', 'tp')
The draws below stay inside these ranges and needn't reach their ends.
All inputs are finite; a program needn't handle non-finite values.
Results may differ from the reference program's by a relative error of at most 0.01.
Values may be sent and summed in bfloat16 or wider, within the bound.
A program may use at most 64 MiB of HBM per device.

```python
import math
import jax
import jax.numpy as jnp
from jax import lax

D = 4096
POOL_W = 1024
POOL_GW = 256
SSD_W = 2048
MIXER_HEAD_SIZE = 64
HEADS = 32
GROUPS = 8
STATE = 128
BLOCK = 128
TOK_DEV = 128
TOKENS = 8192


def draw_decay_log(key, part):
    pick_key, fast_key, slow_key = jax.random.split(jax.random.fold_in(key, 11), 3)
    fast_share = 0.5
    is_fast = jax.random.uniform(pick_key, (2, HEADS), jnp.float32) < fast_share
    fast_rate = jax.random.uniform(fast_key, (2, HEADS), jnp.float32, math.log(0.02), math.log(0.06))
    slow_rate = jax.random.uniform(slow_key, (2, HEADS), jnp.float32, math.log(0.1), math.log(0.4)) - math.log(TOKENS)
    return jnp.where(is_fast, fast_rate, slow_rate)


def draw_leak(key, part):
    level_key, spot_key, size_key = jax.random.split(jax.random.fold_in(key, 23), 3)
    block_count = TOKENS // TOK_DEV
    level = jnp.exp(jax.random.uniform(level_key, (block_count, 2, HEADS), jnp.float32, math.log(0.1), math.log(0.4))) / TOKENS
    starting_shift = jnp.repeat(level, TOK_DEV, axis=0)
    probe_locations = jax.random.randint(spot_key, (2, 2, HEADS), 0, TOKENS)
    overall_quantity = -jnp.log(1.0 - jax.random.uniform(size_key, (2, 2, HEADS), jnp.float32, 0.2, 0.5))
    element_index = jnp.arange(TOKENS, dtype=jnp.int32)[:, None, None, None]
    cluster_sets = jnp.sum(jnp.where(element_index == probe_locations[None], overall_quantity[None], 0.0), axis=1)
    return (starting_shift + cluster_sets).astype(jnp.float32)


def levels(rng, dims, cuts, low, top_value):
    def one(dim, blocks):
        steps = jax.random.uniform(jax.random.fold_in(jax.random.fold_in(rng, 6), dim), (blocks,), jnp.float32, low / len(cuts), top_value / len(cuts))
        return jnp.repeat(jnp.exp(steps), dims[dim] // blocks).reshape((-1,) + (1,) * (len(dims) - dim - 1))

    level = one(*cuts[0])
    for cut in cuts[1:]:
        level = level * one(*cut)
    return level


def noise(rng, dims, spread, limit, pieces=(), kind=jnp.bfloat16):
    values = spread * jax.random.normal(rng, dims, jnp.float32)
    if pieces:
        values = values * levels(rng, dims, pieces, -0.22, 0.18)
    return jnp.clip(values, -limit, limit).astype(kind)


def setup_inputs(seed: int = 0) -> dict:
    key_list = jax.random.split(jax.random.key(seed), 17)
    tokens = noise(key_list[0], (TOKENS, D), 1.0, 6.0, ((0, 64),))
    norm_gain = jnp.clip(1.0 + 0.18 * jax.random.normal(key_list[1], (D,), jnp.float32), 0.099609375, 1.8984375).astype(jnp.bfloat16)
    w_pool_in = noise(key_list[2], (D, POOL_W), D ** -0.5, 0.09375, ((0, 64), (1, 8)))
    w_x = noise(key_list[3], (D, SSD_W), D ** -0.5, 0.09375, ((0, 64), (1, 8)))
    w_z = noise(key_list[4], (D, SSD_W), D ** -0.5, 0.09375, ((0, 64), (1, 8)))
    w_b = noise(key_list[5], (D, GROUPS * STATE), D ** -0.5, 0.09375, ((0, 64), (1, 8)))
    w_c = noise(key_list[6], (D, GROUPS * STATE), D ** -0.5, 0.09375, ((0, 64), (1, 8)))
    w_dt = noise(key_list[7], (D, 2, HEADS), D ** -0.5, 0.09375, ((2, 8),))
    conv_x = noise(key_list[8], (3, SSD_W), 3 ** -0.5, 3.5, ((1, 8),))
    conv_b = noise(key_list[9], (3, GROUPS * STATE), 3 ** -0.5, 3.5, ((1, 8),))
    output_map_taps = noise(key_list[10], (3, GROUPS * STATE), 3 ** -0.5, 3.5, ((1, 8),))
    decay_log = draw_decay_log(jax.random.fold_in(key_list[16], 71), 0)
    leak = draw_leak(jax.random.fold_in(key_list[16], 71), 0)
    init_state = noise(key_list[13], (2, HEADS, MIXER_HEAD_SIZE, STATE), (0.3 * TOKENS ** 0.5), 162.9174, ((1, 8),), jnp.float32)
    head_gain = jnp.clip(1.0 + 0.18 * jax.random.normal(key_list[14], (SSD_W,), jnp.float32), 0.099609375, 1.8984375).astype(jnp.bfloat16)
    w_out = noise(key_list[15], (POOL_W + SSD_W, D), (POOL_W + SSD_W) ** -0.5, 0.109375, ((0, 64), (1, 8)))
    return dict(tokens=tokens, norm_gain=norm_gain, w_pool_in=w_pool_in, w_x=w_x, w_z=w_z, w_b=w_b, w_c=w_c, w_dt=w_dt, conv_x=conv_x, conv_b=conv_b, output_map_taps=output_map_taps, decay_log=decay_log, leak=leak, init_state=init_state, head_gain=head_gain, w_out=w_out)


epsilon = 1e-06
windows = (2, 4, 8, 16)
pool_reach = 8

def rounded(value):
    return lax.optimization_barrier(value.astype(jnp.bfloat16))

def window_means(padded, first_pos, seq_total, channel_group):
    count_rows = padded.shape[0] - 2 * pool_reach
    prefix = jnp.concatenate([jnp.zeros((1, padded.shape[1]), jnp.float32), jnp.cumsum(padded, axis=0)], axis=0)
    element_index = first_pos + jnp.arange(count_rows, dtype=jnp.int32)
    result = jnp.zeros((count_rows, padded.shape[1]), jnp.float32)
    for group_id, window in enumerate(windows):
        low_reach = window // 2
        high_reach = window - 1 - low_reach
        upper_sum = prefix[pool_reach + high_reach + 1:pool_reach + high_reach + 1 + count_rows]
        lower_sum = prefix[pool_reach - low_reach:pool_reach - low_reach + count_rows]
        tallied_items = jnp.minimum(element_index + high_reach, seq_total - 1) - jnp.maximum(element_index - low_reach, 0) + 1
        means = (upper_sum - lower_sum) / tallied_items.astype(jnp.float32)[:, None]
        result = jnp.where(channel_group[None, :] == group_id, means, result)
    return result

def conv_silu(extended, conv_weight):
    weight = conv_weight.astype(jnp.float32)
    values = extended.astype(jnp.float32)
    summed = values[:-2] * weight[0] + values[1:-1] * weight[1] + values[2:] * weight[2]
    return jax.nn.silu(summed)

def ssd_block(state_in, inputs):
    x_blk, b_blk, c_blk, dt_blk, decay_blk = inputs
    block_length = x_blk.shape[0]
    cumul = jnp.cumsum(decay_blk, axis=0)
    scores = jnp.einsum('ign,kgn->gik', c_blk.astype(jnp.float32), b_blk.astype(jnp.float32))
    index = jnp.arange(block_length)
    below = index[:, None] >= index[None, :]
    cumul_t = jnp.transpose(cumul, (1, 2, 0))
    gap_log = cumul_t[:, :, :, None] - cumul_t[:, :, None, :]
    decay_mat = jnp.exp(jnp.where(below, gap_log, -jnp.inf))
    dt_t = jnp.transpose(dt_blk, (1, 2, 0))
    mixing = rounded(scores[:, None] * decay_mat * dt_t[:, :, None, :])
    inner = jnp.einsum('gjik,kgjp->igjp', mixing.astype(jnp.float32), x_blk.astype(jnp.float32))
    carried = jnp.exp(cumul)[..., None] * jnp.einsum('ign,gjpn->igjp', c_blk.astype(jnp.float32), state_in, precision=lax.Precision.HIGHEST)
    to_end = jnp.exp(cumul[-1:] - cumul) * dt_blk
    scaled_b = rounded(to_end[..., None] * b_blk.astype(jnp.float32)[:, :, None, :])
    state_out = jnp.exp(cumul[-1])[..., None, None] * state_in + jnp.einsum('kgjp,kgjn->gjpn', x_blk.astype(jnp.float32), scaled_b.astype(jnp.float32))
    return (state_out, inner + carried)

def run_direction(heads_x, b_groups, c_groups, step_dir, decay_dir, start_state):
    block_count = heads_x.shape[0] // BLOCK

    def to_blocks(values_in):
        return values_in.reshape((block_count, BLOCK) + values_in.shape[1:])
    final_state, outputs = lax.scan(ssd_block, start_state, (to_blocks(heads_x), to_blocks(b_groups), to_blocks(c_groups), to_blocks(step_dir), to_blocks(decay_dir)))
    return outputs.reshape(heads_x.shape)

def reference(tokens, norm_gain, w_pool_in, w_x, w_z, w_b, w_c, w_dt, conv_x, conv_b, output_map_taps, decay_log, leak, init_state, head_gain, w_out):
    seq_total = tokens.shape[0]
    token_f = tokens.astype(jnp.float32)
    normed = rounded(token_f * lax.rsqrt(lax.optimization_barrier(jnp.mean(token_f * token_f, axis=1, keepdims=True)) + epsilon) * norm_gain.astype(jnp.float32))

    def project(weight):
        return jnp.dot(normed, weight, preferred_element_type=jnp.float32)
    pool_in = rounded(project(w_pool_in))
    ssd_x = rounded(project(w_x))
    gate_z = rounded(project(w_z))
    ssd_b = rounded(project(w_b))
    ssd_c = rounded(project(w_c))
    dt_raw = project(w_dt.reshape(w_dt.shape[0], 2 * HEADS)).reshape(seq_total, 2, HEADS)
    channel_group = jnp.arange(POOL_W, dtype=jnp.int32) // POOL_GW
    padded = jnp.pad(pool_in.astype(jnp.float32), ((pool_reach, pool_reach), (0, 0)))
    pooled = rounded(window_means(padded, 0, seq_total, channel_group) - pool_in.astype(jnp.float32))
    stacked = jnp.concatenate([ssd_x, ssd_b, ssd_c], axis=1)
    conv_weight = jnp.concatenate([conv_x, conv_b, output_map_taps], axis=1)
    convolved = rounded(conv_silu(jnp.pad(stacked, ((1, 1), (0, 0))), conv_weight))
    per_group = HEADS // GROUPS
    heads_x = convolved[:, :SSD_W].reshape(seq_total, GROUPS, per_group, MIXER_HEAD_SIZE)
    b_groups = convolved[:, SSD_W:SSD_W + GROUPS * STATE].reshape(seq_total, GROUPS, STATE)
    c_groups = convolved[:, SSD_W + GROUPS * STATE:].reshape(seq_total, GROUPS, STATE)
    step_size = jax.nn.softplus(dt_raw)
    log_decay = -step_size * jnp.exp(decay_log)[None] - leak
    step_size = step_size.reshape(seq_total, 2, GROUPS, per_group)
    log_decay = log_decay.reshape(seq_total, 2, GROUPS, per_group)
    start = init_state.reshape(2, GROUPS, per_group, MIXER_HEAD_SIZE, STATE)
    forward = run_direction(heads_x, b_groups, c_groups, step_size[:, 0], log_decay[:, 0], start[0])
    backward = run_direction(heads_x[::-1], b_groups[::-1], c_groups[::-1], step_size[::-1, 1], log_decay[::-1, 1], start[1])[::-1]
    gated = (forward + backward).reshape(seq_total, HEADS, MIXER_HEAD_SIZE) * jax.nn.silu(gate_z.astype(jnp.float32)).reshape(seq_total, HEADS, MIXER_HEAD_SIZE)
    head_norm = gated * lax.rsqrt(lax.optimization_barrier(jnp.mean(gated * gated, axis=2, keepdims=True)) + epsilon)
    ssd_y = rounded(head_norm.reshape(seq_total, SSD_W) * head_gain.astype(jnp.float32))
    joined = jnp.concatenate([pooled, ssd_y], axis=1)
    return jnp.dot(joined, w_out, preferred_element_type=jnp.float32).astype(jnp.bfloat16)
```

```python
import functools

import jax
import jax.numpy as jnp
from jax import lax
from jax.experimental import pallas as pl
from jax.experimental.pallas import tpu as pltpu
from jax.sharding import Mesh
from jax.sharding import PartitionSpec as P

MESH = pl.DeviceIdType.MESH
F32 = jnp.float32
BF16 = jnp.bfloat16

POOL_GW = 256
HEAD = 64
BLOCK = 128
EDGE = 16
EPS = 1e-06
PIECES = 4
CHUNKS = 4


def silu(v):
    return v / (1.0 + jnp.exp(-v))


def dot_t(a, b, precision=None):
    return lax.dot_general(
        a, b, (((1,), (1,)), ((), ())), precision=precision, preferred_element_type=F32
    )


def split3(v):
    hi = v.astype(BF16).astype(F32)
    mid = (v - hi).astype(BF16).astype(F32)
    lo = (v - hi - mid).astype(BF16).astype(F32)
    return hi, mid, lo


def decay_tile(fwd, bwd):
    row = lax.broadcasted_iota(jnp.int32, (16, 128), 0)
    tile = jnp.zeros((16, 128), F32)
    for k, part in enumerate(split3(fwd) + split3(bwd)):
        tile = jnp.where(row == k, jnp.broadcast_to(part, (16, 128)), tile)
    return tile.astype(BF16)


def decays_of(tile):
    t = tile.astype(F32)
    return t[0:1] + t[1:2] + t[2:3], t[3:4] + t[4:5] + t[5:6]


def kernel(
    dims,
    tok_hbm, gain, wp, wx, wz, wb, wc, wdt, cx, cb, cc, alog, leak, init, hgain, wo,
    out,
    tokv, normed, tsend, tall, wall, oall,
    r1s, r1r, r1o, r2s, r2r, r2o, conv, initv,
    us, ur, vs, vr, hs, hr, ds, dr, es, er,
    yin, heads, pmine, smine, joined,
    lsem, wss, wrs, oss, ors, tss, trs, hls, hlr,
    r1ss, r1rs, r2ss, r2rs, uss, urs, vss, vrs, hss, hrs, dss, drs, ess, ers,
    pss, prs, sss, srs, bss, brs,
):
    nz, ny, nx, nc = dims
    nq = 4
    nzh = nz // nq
    half = nz // 2
    ntp = nx * nc
    d_model = tok_hbm.shape[1]
    kq = d_model // ny
    wr = wp.shape[0]
    orow = wo.shape[0]
    z = lax.axis_index("z")
    y = lax.axis_index("y")
    xi = lax.axis_index("x")
    ci = lax.axis_index("c")
    t = xi * nc + ci
    zl = lax.rem(z, nq)
    zh = lax.div(z, nq)
    up = lax.rem(z + 1, nz)
    down = lax.rem(z + nz - 1, nz)

    def ypeer(k):
        return lax.rem(y + k, ny)

    def remote(src, dst, ssem, rsem, dev):
        return pltpu.make_async_remote_copy(
            src_ref=src, dst_ref=dst, send_sem=ssem, recv_sem=rsem,
            device_id=dev, device_id_type=MESH,
        )

    wrows = pl.ds(pl.multiple_of(z * wr, wr), wr)
    locals_ = [
        pltpu.make_async_copy(wx, wall.at[wrows, pl.ds(0, 256)], lsem.at[0]),
        pltpu.make_async_copy(wb, wall.at[wrows, pl.ds(256, 128)], lsem.at[1]),
        pltpu.make_async_copy(wc, wall.at[wrows, pl.ds(384, 128)], lsem.at[2]),
        pltpu.make_async_copy(wz, wall.at[wrows, pl.ds(512, 256)], lsem.at[3]),
        pltpu.make_async_copy(wp, wall.at[wrows, pl.ds(768, 128)], lsem.at[4]),
        pltpu.make_async_copy(tok_hbm, tokv, lsem.at[5]),
        pltpu.make_async_copy(wo, oall.at[z, y], lsem.at[6]),
        pltpu.make_async_copy(init, initv, lsem.at[7]),
    ]
    for c in locals_:
        c.start()
    barrier = pltpu.get_barrier_semaphore()
    count = 0
    for dz in (0, 1, nz - 1):
        for k in range(ny):
            if dz == 0 and k == 0:
                continue
            pl.semaphore_signal(
                barrier, inc=1, device_id={"z": lax.rem(z + dz, nz), "y": ypeer(k)}, device_id_type=MESH
            )
            count += 1

    def tp_dev(d):
        p = lax.rem(t + d, ntp)
        return {"x": lax.div(p, nc), "c": lax.rem(p, nc)}

    for d in range(1, ntp):
        pl.semaphore_signal(barrier, inc=1, device_id=tp_dev(d), device_id_type=MESH)
        count += 1
    for c in locals_[:5]:
        c.wait()
    pl.semaphore_wait(barrier, count)

    def ring_copy(k, way, p, sending):
        shift = k if sending else k + 1
        slot = lax.rem(z + nz - shift, nz) if way == 0 else lax.rem(z + shift, nz)
        rows = pl.ds(pl.multiple_of(slot * wr + (wr // PIECES) * p, wr // PIECES), wr // PIECES)
        return remote(
            wall.at[rows], wall.at[rows], wss.at[way, k, p], wrs.at[way, k, p],
            {"z": up if way == 0 else down},
        )

    def in_ring(k, way, p):
        return k < half - 1 or (way == 0) == (p < PIECES // 2)

    def ring_step(k):
        for p in range(PIECES):
            for way in (0, 1):
                if k > 0:
                    if not in_ring(k - 1, way, p):
                        continue
                    ring_copy(k - 1, way, p, False).wait_recv()
                if k < half and in_ring(k, way, p):
                    ring_copy(k, way, p, True).start()

    def oring_copy(k, way, sending):
        shift = k if sending else k + 1
        slot = lax.rem(z + nz - shift, nz) if way == 0 else lax.rem(z + shift, nz)
        return remote(
            oall.at[slot, y], oall.at[slot, y], oss.at[way, k], ors.at[way, k],
            {"z": up if way == 0 else down},
        )

    def in_oring(k, way):
        return k < half - 1 or way == 0

    def oring_step(k):
        for way in (0, 1):
            if k > 0:
                if not in_oring(k - 1, way):
                    continue
                oring_copy(k - 1, way, False).wait_recv()
            if k < half and in_oring(k, way):
                oring_copy(k, way, True).start()

    def bulk_copy(k, c, sending):
        col = y if sending else lax.rem(y + ny - k, ny)
        span = pl.ds(c * (nz // CHUNKS), nz // CHUNKS)
        return remote(
            oall.at[span, col], oall.at[span, col], bss.at[k - 1, c], brs.at[k - 1, c],
            {"y": ypeer(k)},
        )

    ring_step(0)

    locals_[5].wait()
    lane = lax.broadcasted_iota(jnp.int32, (16, 128), 1)

    def norm_rows(i, carry):
        rows = pl.ds(pl.multiple_of(16 * i, 16), 16)
        v = tokv[rows, :].astype(F32)
        ms = jnp.mean(v * v, axis=1, keepdims=True)
        n = (v * lax.rsqrt(ms + EPS) * gain[...].astype(F32)).astype(BF16)
        normed[rows, :] = n
        nf = n.astype(F32)
        for m in range(kq // 128):
            for h in range(ny // 2):
                a0 = wr * ny * (2 * m) + 128 * h
                a1 = wr * ny * (2 * m + 1) + 128 * h
                t0 = nf[:, a0 : a0 + 128]
                t1 = nf[:, a1 : a1 + 128]
                even = jnp.where(lane < 64, t0, pltpu.roll(t1, 64, 1))
                odd = jnp.where(lane < 64, pltpu.roll(t0, 64, 1), t1)
                tsend[2 * h, rows, 128 * m : 128 * m + 128] = even.astype(BF16)
                tsend[2 * h + 1, rows, 128 * m : 128 * m + 128] = odd.astype(BF16)
        return carry

    lax.fori_loop(0, 128 // 16, norm_rows, 0)

    def trows(src):
        return pl.ds(pl.multiple_of(EDGE + BLOCK * src, 16), BLOCK)

    def tok_copy(k, sending):
        src = y if sending else lax.rem(y + ny - k, ny)
        return remote(
            tsend.at[ypeer(k)], tall.at[trows(src)], tss.at[k - 1], trs.at[k - 1], {"y": ypeer(k)}
        )

    top = EDGE + BLOCK * ny

    def left_edge(k):
        return remote(
            tsend.at[k, pl.ds(BLOCK - EDGE, EDGE)], tall.at[pl.ds(0, EDGE)], hls.at[k], hlr.at[0],
            {"z": up, "y": k},
        )

    def right_edge(k):
        return remote(
            tsend.at[k, pl.ds(0, EDGE)], tall.at[pl.ds(top, EDGE)], hls.at[k], hlr.at[1],
            {"z": down, "y": k},
        )

    for k in (2, 1, 3):
        tok_copy(k, True).start()
    sends_left = jnp.logical_and(y == ny - 1, z < nz - 1)
    sends_right = jnp.logical_and(y == 0, z > 0)

    @pl.when(sends_left)
    def _():
        for k in range(ny):
            left_edge(k).start()

    @pl.when(sends_right)
    def _():
        for k in range(ny):
            right_edge(k).start()

    mine = pltpu.make_async_copy(tsend.at[y], tall.at[trows(y)], lsem.at[8])
    mine.start()

    @pl.when(z == 0)
    def _():
        tall[pl.ds(0, EDGE), :] = jnp.zeros((EDGE, kq), BF16)

    @pl.when(z == nz - 1)
    def _():
        tall[pl.ds(top, EDGE), :] = jnp.zeros((EDGE, kq), BF16)

    ring_step(1)
    dt = dot_t(wdt[...], normed[...])
    step = jnp.maximum(dt, 0.0) + jnp.log1p(jnp.exp(-jnp.abs(dt)))
    log_decay = -step * jnp.exp(alog[...]) - leak[...]
    ii = lax.broadcasted_iota(jnp.int32, (BLOCK, BLOCK), 0)
    jj = lax.broadcasted_iota(jnp.int32, (BLOCK, BLOCK), 1)
    low = ii >= jj
    upm = ii <= jj
    hp = lax.Precision.HIGHEST
    sum_f = jnp.dot(log_decay, upm.astype(F32), precision=hp, preferred_element_type=F32)
    sum_b = jnp.dot(log_decay, low.astype(F32), precision=hp, preferred_element_type=F32)
    row8 = lax.broadcasted_iota(jnp.int32, (8, BLOCK), 0)
    cum_t = jnp.where(row8 < 4, sum_f, sum_b)
    tot = jnp.where(
        row8 < 4,
        jnp.broadcast_to(sum_f[:, BLOCK - 1 : BLOCK], (8, BLOCK)),
        jnp.broadcast_to(sum_b[:, 0:1], (8, BLOCK)),
    )
    to_end_t = jnp.exp(tot - cum_t) * step
    stacked = jnp.concatenate([cum_t, to_end_t, jnp.zeros((112, BLOCK), F32)], axis=0)
    cols = jnp.transpose(stacked)

    for k in range(2, half):
        ring_step(k)
    locals_[6].wait()
    oring_step(0)
    ring_step(half)

    for k in (1, 2, 3):
        tok_copy(k, False).wait_recv()
    mine.wait()

    @pl.when(z > 0)
    def _():
        left_edge(0).wait_recv()

    @pl.when(z < nz - 1)
    def _():
        right_edge(0).wait_recv()

    ext = BLOCK + 2 * EDGE

    def part(k, lo, hi):
        rows = pl.ds(pl.multiple_of(BLOCK * ypeer(k), 16), ext)
        return jnp.dot(tall[rows, :], wall[:, lo:hi], preferred_element_type=F32)

    def r1_copy(k):
        return remote(r1s.at[k - 1], r1r.at[k - 1], r1ss.at[k - 1], r1rs.at[k - 1], {"y": ypeer(k)})

    def r2_copy(k):
        return remote(r2s.at[k - 1], r2r.at[k - 1], r2ss.at[k - 1], r2rs.at[k - 1], {"y": ypeer(k)})

    for k in (2, 1, 3):
        r1s[k - 1] = part(k, 0, 512).astype(BF16)
        r1_copy(k).start()
    for k in (2, 1, 3):
        r2s[k - 1] = part(k, 512, 896).astype(BF16)
        r2_copy(k).start()
    r1o[...] = part(0, 0, 512)
    r2o[...] = part(0, 512, 896)
    for k in range(1, 3):
        oring_step(k)

    for k in (1, 3, 2):
        r1_copy(k).wait_recv()
    total = r1o[...]
    for k in range(3):
        total = total + r1r[k].astype(F32)
    conv[...] = total.astype(BF16).astype(F32)
    taps = jnp.concatenate([cx[...], cb[...], cc[...]], axis=1).astype(F32)
    mixed = (
        conv[EDGE - 1 : EDGE - 1 + BLOCK, :] * taps[0:1]
        + conv[EDGE : EDGE + BLOCK, :] * taps[1:2]
        + conv[EDGE + 1 : EDGE + 1 + BLOCK, :] * taps[2:3]
    )
    cv = silu(mixed)
    xf = cv[:, 0:256].astype(BF16)
    bg = cv[:, 256:384].astype(BF16)
    cg = cv[:, 384:512].astype(BF16)
    bf = bg.astype(F32)
    xt = jnp.transpose(xf.astype(F32)).astype(BF16)

    def up_copy(k):
        return remote(us.at[ypeer(k)], ur.at[y], uss.at[k - 1], urs.at[k - 1], {"y": ypeer(k)})

    def up_recv(k):
        src = lax.rem(y + ny - k, ny)
        return remote(us.at[ypeer(k)], ur.at[src], uss.at[k - 1], urs.at[k - 1], {"y": ypeer(k)})

    for h in range(4):
        sb = jnp.concatenate(
            [(cols[:, 8 + h : 9 + h] * bf).astype(BF16), (cols[:, 12 + h : 13 + h] * bf).astype(BF16)], axis=1
        )
        st = jnp.dot(xt[64 * h : 64 * h + 64], sb, preferred_element_type=F32)
        us[h, 0:64, :] = st[:, 0:128].astype(BF16)
        us[h, 64:128, :] = st[:, 128:256].astype(BF16)
        us[h, 128:144, :] = decay_tile(tot[h : h + 1], tot[4 + h : 5 + h])
    for k in (2, 1, 3):
        up_copy(k).start()
    ur[pl.ds(y, 1)] = us[pl.ds(y, 1)]

    scores = dot_t(cg, bg)
    for h in range(4):
        gf = cols[:, h : h + 1] - cum_t[h : h + 1]
        gb = cols[:, 4 + h : 5 + h] - cum_t[4 + h : 5 + h]
        mf = scores * jnp.exp(jnp.where(low, gf, -jnp.inf)) * step[h : h + 1]
        mb = scores * jnp.exp(jnp.where(upm, gb, -jnp.inf)) * step[4 + h : 5 + h]
        mm = jnp.concatenate([mf.astype(BF16), mb.astype(BF16)], axis=1)
        xh = xf[:, 64 * h : 64 * h + 64]
        yin[:, 64 * h : 64 * h + 64] = jnp.dot(
            mm, jnp.concatenate([xh, xh], axis=0), preferred_element_type=F32
        )
    oring_step(3)

    for k in (1, 3, 2):
        up_recv(k).wait_recv()
    lf, lb = zip(*[decays_of(ur[j, 128:144, :]) for j in range(ny)])

    def totals(sf, sb, lf, lb):
        n = len(sf)
        gf, gb = sf[0], sb[n - 1]
        for j in range(1, n):
            gf = jnp.exp(lf[j]) * gf + sf[j]
            gb = jnp.exp(lb[n - 1 - j]) * gb + sb[n - 1 - j]
        return gf, gb, functools.reduce(lambda a, b: a + b, lf), functools.reduce(lambda a, b: a + b, lb)

    ysf = [ur[j, 0:64, :].astype(F32) for j in range(ny)]
    ysb = [ur[j, 64:128, :].astype(F32) for j in range(ny)]
    gf, gb, glf, glb = totals(ysf, ysb, lf, lb)
    tile = decay_tile(glf, glb)
    for q in range(nq):
        vs[q, 0:16, :] = gf[16 * q : 16 * q + 16].astype(BF16)
        vs[q, 16:32, :] = gb[16 * q : 16 * q + 16].astype(BF16)
        vs[q, 32:48, :] = tile

    def zq(k):
        return lax.rem(zl + k, nq)

    def v_copy(k, sending):
        src = zl if sending else lax.rem(zl + nq - k, nq)
        return remote(vs.at[zq(k)], vr.at[src], vss.at[k - 1], vrs.at[k - 1], {"z": zh * nq + zq(k)})

    for k in (2, 1, 3):
        v_copy(k, True).start()
    vr[pl.ds(zl, 1)] = vs[pl.ds(zl, 1)]
    oring_step(4)
    for k in (1, 3, 2):
        v_copy(k, False).wait_recv()
    zf, zb = zip(*[decays_of(vr[j, 32:48, :]) for j in range(nq)])
    zsf = [vr[j, 0:16, :].astype(F32) for j in range(nq)]
    zsb = [vr[j, 16:32, :].astype(F32) for j in range(nq)]
    hf, hb, hlf, hlb = totals(zsf, zsb, zf, zb)
    hs[0:16, :] = hf.astype(BF16)
    hs[16:32, :] = hb.astype(BF16)
    hs[32:48, :] = decay_tile(hlf, hlb)

    def h_copy(k, sending):
        src = zh if sending else lax.rem(zh + nzh - k, nzh)
        return remote(
            hs, hr.at[src], hss.at[k - 1], hrs.at[k - 1], {"z": lax.rem(zh + k, nzh) * nq + zl}
        )

    for k in range(1, nzh):
        h_copy(k, True).start()
    hr[pl.ds(zh, 1)] = hs[...].reshape(1, 48, 128)

    for k in (1, 3, 2):
        r2_copy(k).wait_recv()
    total = r2o[...]
    for k in range(3):
        total = total + r2r[k].astype(F32)
    pin = total[:, 256:384].astype(BF16).astype(F32)
    r2o[:, 0:256] = silu(total[:, 0:256].astype(BF16).astype(F32))

    def moved(v, by):
        return pltpu.roll(v, by % ext, 0)

    s2 = pin + moved(pin, 1)
    s4 = moved(s2, 1) + moved(s2, -1)
    s8 = moved(s4, 2) + moved(s4, -2)
    s16 = moved(s8, 4) + moved(s8, -4)
    group = lax.div(t * BLOCK, POOL_GW)
    lo_reach = lax.shift_left(jnp.int32(1), group)
    hi_reach = lo_reach - 1
    sums = jnp.where(group == 0, s2, jnp.where(group == 1, s4, jnp.where(group == 2, s8, s16)))
    first = (z * ny + y) * BLOCK
    pos = first + lax.broadcasted_iota(jnp.int32, (BLOCK, 128), 0)
    tally = jnp.minimum(pos + hi_reach, nz * ny * BLOCK - 1) - jnp.maximum(pos - lo_reach, 0) + 1
    own_rows = slice(EDGE, EDGE + BLOCK)
    pmine[...] = (sums[own_rows] / tally.astype(F32) - pin[own_rows]).astype(BF16)

    def p_copy(d, sending):
        src = t if sending else lax.rem(t + ntp - d, ntp)
        at = pl.ds(pl.multiple_of(128 * src, 128), 128)
        return remote(pmine, joined.at[:, at], pss.at[d - 1], prs.at[d - 1], tp_dev(d))

    def s_copy(d, sending):
        src = t if sending else lax.rem(t + ntp - d, ntp)
        at = pl.ds(pl.multiple_of(128 * ntp + 256 * src, 128), 256)
        return remote(smine, joined.at[:, at], sss.at[d - 1], srs.at[d - 1], tp_dev(d))

    for d in range(1, ntp):
        p_copy(d, True).start()
    joined[:, pl.ds(pl.multiple_of(128 * t, 128), 128)] = pmine[...]
    for k in range(5, half + 1):
        oring_step(k)
    for c in range(CHUNKS):
        for k in (2, 1, 3):
            bulk_copy(k, c, True).start()

    for k in range(1, nzh):
        h_copy(k, False).wait_recv()
    locals_[7].wait()
    quarter = pl.ds(pl.multiple_of(16 * zl, 16), 16)
    ef = initv[0, pl.ds(y, 1), quarter, :].reshape(16, 128)
    eb = initv[1, pl.ds(y, 1), quarter, :].reshape(16, 128)
    inf, inb = ef, eb
    hd = [decays_of(hr[j, 32:48, :]) for j in range(nzh)]
    for j in range(nzh):
        inf = jnp.where(zh == j, ef, inf)
        ef = jnp.exp(hd[j][0]) * ef + hr[j, 0:16, :].astype(F32)
        b = nzh - 1 - j
        inb = jnp.where(zh == b, eb, inb)
        eb = jnp.exp(hd[b][1]) * eb + hr[b, 16:32, :].astype(F32)
    for j in range(nq):
        ds[j, 0:16, :] = inf.astype(BF16)
        inf = jnp.exp(zf[j]) * inf + zsf[j]
        b = nq - 1 - j
        ds[b, 16:32, :] = inb.astype(BF16)
        inb = jnp.exp(zb[b]) * inb + zsb[b]

    def d_copy(k, sending):
        src = zl if sending else lax.rem(zl + nq - k, nq)
        return remote(ds.at[zq(k)], dr.at[src], dss.at[k - 1], drs.at[k - 1], {"z": zh * nq + zq(k)})

    for k in (2, 1, 3):
        d_copy(k, True).start()
    dr[pl.ds(zl, 1)] = ds[pl.ds(zl, 1)]
    for k in (1, 3, 2):
        d_copy(k, False).wait_recv()
    ef = jnp.concatenate([dr[q, 0:16, :] for q in range(nq)], axis=0).astype(F32)
    eb = jnp.concatenate([dr[q, 16:32, :] for q in range(nq)], axis=0).astype(F32)
    for j in range(ny):
        es[j, 0:64, :] = ef.astype(BF16)
        ef = jnp.exp(lf[j]) * ef + ysf[j]
        b = ny - 1 - j
        es[b, 64:128, :] = eb.astype(BF16)
        eb = jnp.exp(lb[b]) * eb + ysb[b]

    def e_copy(k, sending):
        src = y if sending else lax.rem(y + ny - k, ny)
        return remote(es.at[ypeer(k)], er.at[src], ess.at[k - 1], ers.at[k - 1], {"y": ypeer(k)})

    for k in (2, 1, 3):
        e_copy(k, True).start()
    er[pl.ds(y, 1)] = es[pl.ds(y, 1)]
    for k in (1, 3, 2):
        e_copy(k, False).wait_recv()

    for h in range(4):
        ch = dot_t(cg, er[h])
        v = (
            yin[:, 64 * h : 64 * h + 64]
            + jnp.exp(cols[:, h : h + 1]) * ch[:, 0:64]
            + jnp.exp(cols[:, 4 + h : 5 + h]) * ch[:, 64:128]
        )
        v = v * r2o[EDGE : EDGE + BLOCK, 64 * h : 64 * h + 64]
        v = v * lax.rsqrt(jnp.mean(v * v, axis=1, keepdims=True) + EPS)
        heads[:, 64 * h : 64 * h + 64] = v
    smine[...] = (heads[...] * hgain[...].astype(F32)).astype(BF16)
    for d in range(1, ntp):
        s_copy(d, True).start()
    joined[:, pl.ds(pl.multiple_of(128 * ntp + 256 * t, 128), 256)] = smine[...]
    for k in (1, 3, 2):
        for c in range(CHUNKS):
            bulk_copy(k, c, False).wait_recv()
    for d in range(1, ntp):
        p_copy(d, False).wait_recv()
    for d in range(1, ntp):
        s_copy(d, False).wait_recv()
    rows = ntp * 384
    acc = jnp.dot(
        joined[...], oall[...].reshape(rows, oall.shape[3]), preferred_element_type=F32
    )
    out[...] = acc.astype(BF16)

    for k in range(half):
        for way in (0, 1):
            for p in range(PIECES):
                if in_ring(k, way, p):
                    ring_copy(k, way, p, True).wait_send()
            if in_oring(k, way):
                oring_copy(k, way, True).wait_send()

    @pl.when(sends_left)
    def _():
        for k in range(ny):
            left_edge(k).wait_send()

    @pl.when(sends_right)
    def _():
        for k in range(ny):
            right_edge(k).wait_send()

    for k in (1, 2, 3):
        tok_copy(k, True).wait_send()
        r1_copy(k).wait_send()
        r2_copy(k).wait_send()
        up_copy(k).wait_send()
        v_copy(k, True).wait_send()
        d_copy(k, True).wait_send()
        e_copy(k, True).wait_send()
        for c in range(CHUNKS):
            bulk_copy(k, c, True).wait_send()
    for k in range(1, nzh):
        h_copy(k, True).wait_send()
    for d in range(1, ntp):
        p_copy(d, True).wait_send()
        s_copy(d, True).wait_send()


def per_device(
    dims,
    tokens, norm_gain, w_pool_in, w_x, w_z, w_b, w_c, w_dt, conv_x, conv_b, output_map_taps,
    decay_log, leak, init_state, head_gain, w_out,
):
    nz, ny, nx, nc = dims
    ntp = nx * nc
    d_model = tokens.shape[1]
    kq = d_model // ny
    half = nz // 2
    nzh = nz // 4
    ext = BLOCK + 2 * EDGE
    f_out = w_out.shape[1]
    wdt_t = jnp.transpose(w_dt, (1, 2, 0)).reshape(8, d_model)
    leak_t = jnp.transpose(leak, (1, 2, 0)).reshape(8, BLOCK)
    alog = decay_log.reshape(8, 1)
    any_ = pl.BlockSpec(memory_space=pl.ANY)
    vmem = pl.BlockSpec(memory_space=pltpu.VMEM)
    dma = pltpu.SemaphoreType.DMA

    def v(*shape, dtype=BF16):
        return pltpu.VMEM(shape, dtype)

    scratch = [
        v(BLOCK, d_model), v(BLOCK, d_model), v(ny, BLOCK, kq), v(BLOCK * ny + 2 * EDGE, kq),
        v(kq, 896), v(nz, ny, w_out.shape[0], f_out),
        v(3, ext, 512), v(3, ext, 512), v(ext, 512, dtype=F32),
        v(3, ext, 384), v(3, ext, 384), v(ext, 384, dtype=F32),
        v(ext, 512, dtype=F32), v(2, 4, 64, 128, dtype=F32),
        v(ny, 144, 128), v(ny, 144, 128), v(4, 48, 128), v(4, 48, 128), v(48, 128), v(nzh, 48, 128),
        v(4, 32, 128), v(4, 32, 128), v(ny, 128, 128), v(ny, 128, 128),
        v(BLOCK, 256, dtype=F32), v(BLOCK, 256, dtype=F32), v(BLOCK, 128), v(BLOCK, 256),
        v(BLOCK, 384 * ntp),
        dma((9,)), dma((2, half, PIECES)), dma((2, half, PIECES)), dma((2, half)), dma((2, half)),
        dma((3,)), dma((3,)), dma((ny,)), dma((2,)),
        dma((3,)), dma((3,)), dma((3,)), dma((3,)), dma((3,)), dma((3,)), dma((3,)), dma((3,)),
        dma((max(nzh - 1, 1),)), dma((max(nzh - 1, 1),)), dma((3,)), dma((3,)), dma((3,)), dma((3,)),
        dma((max(ntp - 1, 1),)), dma((max(ntp - 1, 1),)), dma((max(ntp - 1, 1),)), dma((max(ntp - 1, 1),)),
        dma((3, CHUNKS)), dma((3, CHUNKS)),
    ]
    return pl.pallas_call(
        functools.partial(kernel, dims),
        out_shape=jax.ShapeDtypeStruct((BLOCK, f_out), BF16),
        in_specs=[any_, vmem, any_, any_, any_, any_, any_, vmem, vmem, vmem, vmem, vmem, vmem, any_, vmem, any_],
        out_specs=vmem,
        scratch_shapes=scratch,
        compiler_params=pltpu.CompilerParams(
            collective_id=0, has_side_effects=True, vmem_limit_bytes=50 * 1024 * 1024
        ),
        name="layer",
    )(
        tokens, norm_gain.reshape(1, d_model), w_pool_in, w_x, w_z, w_b, w_c, wdt_t,
        conv_x, conv_b, output_map_taps, alog, leak_t, init_state, head_gain.reshape(1, 256), w_out,
    )


def build(devices, dims):
    finer = Mesh(devices.reshape(dims), ("z", "y", "x", "c"))
    sp, tp = ("z", "y"), ("x", "c")
    placed = (
        P(sp, None), P(), P(sp, tp), P(sp, tp), P(sp, tp), P(sp, tp), P(sp, tp), P(None, None, tp),
        P(None, tp), P(None, tp), P(None, tp), P(None, tp), P(sp, None, tp), P(None, tp, None, None),
        P(tp), P(sp, tp),
    )
    return jax.shard_map(
        functools.partial(per_device, dims), mesh=finer, in_specs=placed, out_specs=P(sp, tp), check_vma=False
    )


def solution(mesh):
    return build(mesh.devices, (16, 4, 4, 2))
```
